32 devices in a mesh: sp: 8 (over z, core), tp: 4 (over y, x).
Axes of the slice: x: 2, y: 2, z: 4, core: 2. Of those that a mesh axis runs over, the one named last changes fastest.
Arguments:
- moe_in: bfloat16 [1536, 2048], P('sp'), may hold values from -6 to 6
- cotangent: bfloat16 [1536, 2048], P('sp'), may hold values from -6 to 6
- routing: int32 [1536, 2], P('sp'), may hold values from 0 to 7, as said below
- route_weight: float32 [1536, 2], P('sp'), may hold values from 0.2 to 1
- w_gate: bfloat16 [8, 2048, 2048], P('sp', 'tp'), may hold values from -0.125 to 0.125
- w_up: bfloat16 [8, 2048, 2048], P('sp', 'tp'), may hold values from -0.125 to 0.125
- w_down: bfloat16 [8, 2048, 2048], P('sp', 'tp'), may hold values from -0.125 to 0.125
- gate_b: bfloat16 [1024, 1536], P('tp', 'sp'), may hold values from -6 to 6
- gate_c: bfloat16 [1024, 1536], P('tp', 'sp'), may hold values from -6 to 6
- value_x: bfloat16 [1024, 1536], P('tp', 'sp'), may hold values from -6 to 6
- conv_taps: float32 [3, 1024], P(None, 'tp'), may hold values from -3 to 3
- out_proj: bfloat16 [1024, 2048], P('tp'), may hold values from -0.1875 to 0.1875
Outputs:
- w_gate_grad: bfloat16 [8, 2048, 2048], P('sp', 'tp')
- w_up_grad: bfloat16 [8, 2048, 2048], P('sp', 'tp')
- w_down_grad: bfloat16 [8, 2048, 2048], P('sp', 'tp')
- moe_in_grad: bfloat16 [1536, 2048], P('sp', 'tp')
- proj_grad: float32 [1024, 2048], P('tp', 'sp')
- gate_b_grad: bfloat16 [1024, 1536], P('tp', 'sp')
- gate_c_grad: bfloat16 [1024, 1536], P('tp', 'sp')
- value_x_grad: bfloat16 [1024, 1536], P('tp', 'sp')
The draws below stay inside these ranges and needn't reach their ends.
Inputs may be any that keep to these rules, and one draw needn't show every extreme that they name: `routing`: in each aligned block of 192 rows every expert is named exactly 48 times. The two entries of a row are different experts of one group; group g holds experts g * 2 to g * 2 + 1.
All inputs are finite; a program needn't handle non-finite values.
Results may differ from the reference program's by a relative error of at most 0.025.
Values may be sent and summed in bfloat16 or wider, within the bound.
No kernel may reach another device: no remote copies, remote signals or barrier semaphores. Data moves between devices by JAX's collectives and lax.ppermute only.
A program may use at most 64 MiB of HBM per device.

```python
import jax
import jax.numpy as jnp
from jax import lax

D = 2048
W_A = 1024
HID = 2048
TAPS = 3
GROUPS = 4
TOPK = 2
TOK_DEV = 192
TOKENS = 1536
EXPERTS = 8
CAP = 48
HID_DEV = 512
N_SP = 8
N_TP = 4


def route_block(block_key):
    per_group = EXPERTS // GROUPS
    key_rank, key_shift, key_group, key_local = jax.random.split(block_key, 4)
    rank = jax.random.permutation(key_rank, TOK_DEV).astype(jnp.int32)
    first = rank % EXPERTS
    cycle = rank // EXPERTS
    offset = jax.random.randint(key_shift, (), 0, per_group, dtype=jnp.int32)
    shift = (cycle + offset) % max(per_group - 1, 1)
    group_id = first // per_group
    local_one = first % per_group
    local_two = (local_one + 1 + shift) % per_group
    group_perm = jax.random.permutation(key_group, GROUPS).astype(jnp.int32)
    local_perm = jax.random.permutation(key_local, per_group).astype(jnp.int32)
    expert_one = group_perm[group_id] * per_group + local_perm[local_one]
    expert_two = group_perm[group_id] * per_group + local_perm[local_two]
    return jnp.stack([expert_one, expert_two], axis=1)


def draw_routing(key, part):
    block_keys = jax.random.split(jax.random.fold_in(key, 17), TOKENS // TOK_DEV)
    blocks = jax.vmap(route_block)(block_keys)
    return blocks.reshape(TOKENS, TOPK).astype(jnp.int32)


def with_spikes(array, key, source, target, shards_of, factor):
    owner, partner = [(jnp.arange(array.shape[axis_at]) // (array.shape[axis_at] // shards_of)).reshape([-1 if axis == axis_at else 1 for axis in range(array.ndim)]) for axis_at in (source, target)]
    chosen = jax.random.permutation(key, shards_of)[partner]
    strong = (owner == chosen) | (owner == (partner + shards_of // 2) % shards_of)
    return jnp.where(strong, factor * array, array)


def block_scale(stream_key, shape, shards, smallest, top_value):
    loudness = 1.0
    for position, parts in shards:
        heights = jax.random.uniform(jax.random.fold_in(jax.random.fold_in(stream_key, 6), position), (parts,), jnp.float32, smallest / len(shards), top_value / len(shards))
        loudness = loudness * jnp.repeat(jnp.exp(heights), shape[position] // parts).reshape((-1,) + (1,) * (len(shape) - 1 - position))
    return loudness


def gaussian(stream_key, extent, scale, bound, cuts=(), kind=jnp.bfloat16):
    entries = scale * jax.random.normal(stream_key, extent, jnp.float32)
    if cuts:
        entries = entries * block_scale(stream_key, extent, cuts, -0.22, 0.18)
    return jnp.clip(entries, -bound, bound).astype(kind)


def gaussian_with(key, dims, deviation, most, cuts, heavy, kind=jnp.bfloat16):
    result = deviation * jax.random.normal(key, dims, jnp.float32)
    if cuts:
        result = result * block_scale(key, dims, cuts, -0.22, 0.18)
    return jnp.clip(with_spikes(result, jax.random.fold_in(key, 3), *heavy), -most, most).astype(kind)


def setup_inputs(seed: int = 0) -> dict:
    key_list = jax.random.split(jax.random.key(seed), 13)
    return {
        "moe_in": gaussian(key_list[0], (TOKENS, D), 1.0, 6.0, ((0, 8),)),
        "cotangent": gaussian_with(key_list[1], (TOKENS, D), 1.0, 6.0, ((0, 8),), (0, 1, 8, 2.0)),
        "routing": draw_routing(jax.random.fold_in(key_list[12], 71), 0),
        "route_weight": jnp.clip(0.2 + 0.8 * jax.random.uniform(key_list[3], (TOKENS, TOPK), jnp.float32) ** block_scale(key_list[3], (TOKENS, TOPK), ((0, 8),), -0.2, 0.2), 0.2, 1.0),
        "w_gate": gaussian(key_list[4], (EXPERTS, HID, D), D ** -0.5, 0.125, ((0, 8), (1, 4))),
        "w_up": gaussian(key_list[5], (EXPERTS, HID, D), D ** -0.5, 0.125, ((0, 8), (1, 4))),
        "w_down": gaussian(key_list[6], (EXPERTS, HID, D), HID ** -0.5, 0.125, ((0, 8), (1, 4))),
        "gate_b": gaussian(key_list[7], (W_A, TOKENS), 1.0, 6.0, ((0, 4), (1, 8))),
        "gate_c": gaussian(key_list[8], (W_A, TOKENS), 1.0, 6.0, ((0, 4), (1, 8))),
        "value_x": gaussian(key_list[9], (W_A, TOKENS), 1.0, 6.0, ((0, 4), (1, 8))),
        "conv_taps": gaussian(key_list[10], (TAPS, W_A), 0.6, 3.0, ((1, 4),), jnp.float32),
        "out_proj": gaussian(key_list[11], (W_A, D), W_A ** -0.5, 0.1875, ((0, 4),)),
    }


def reference(moe_in, cotangent, routing, route_weight, w_gate, w_up, w_down, gate_b, gate_c, value_x, conv_taps, out_proj):
    flat_routes = routing.reshape(-1)
    order = jnp.argsort(flat_routes, stable=True).astype(jnp.int32).reshape(EXPERTS, CAP * N_SP)
    weight_flat = route_weight.reshape(-1)
    contract_model = (((1,), (1,)), ((), ()))
    over_rows = (((0,), (0,)), ((), ()))

    def expert(packed):
        index, gate_weight, up_weight, down_weight = packed
        owner = index // TOPK
        arrived = moe_in[owner]
        route_cot = (weight_flat[index][:, None] * cotangent[owner].astype(jnp.float32)).astype(jnp.bfloat16)
        gate_pre = lax.dot_general(arrived, gate_weight, contract_model, preferred_element_type=jnp.float32)
        up_pre = lax.dot_general(arrived, up_weight, contract_model, preferred_element_type=jnp.float32)
        sigmoid_gate = jax.nn.sigmoid(gate_pre)
        hidden = (gate_pre * sigmoid_gate * up_pre).astype(jnp.bfloat16)
        hidden_grad = lax.dot_general(route_cot, down_weight, contract_model, preferred_element_type=jnp.float32)
        gate_grad = (hidden_grad * up_pre * sigmoid_gate * (1.0 + gate_pre * (1.0 - sigmoid_gate))).astype(jnp.bfloat16)
        up_grad = (hidden_grad * gate_pre * sigmoid_gate).astype(jnp.bfloat16)
        gate_wgrad = lax.dot_general(gate_grad, arrived, over_rows, preferred_element_type=jnp.float32).astype(jnp.bfloat16)
        up_wgrad = lax.dot_general(up_grad, arrived, over_rows, preferred_element_type=jnp.float32).astype(jnp.bfloat16)
        down_wgrad = lax.dot_general(hidden, route_cot, over_rows, preferred_element_type=jnp.float32).astype(jnp.bfloat16)
        row_total = gate_grad.shape[0]
        gate_blocks = gate_grad.astype(jnp.float32).reshape(row_total, N_TP, HID_DEV)
        up_blocks = up_grad.astype(jnp.float32).reshape(row_total, N_TP, HID_DEV)
        gate_table = gate_weight.astype(jnp.float32).reshape(N_TP, HID_DEV, D)
        up_table = up_weight.astype(jnp.float32).reshape(N_TP, HID_DEV, D)
        partial_value = jnp.einsum("rbh,bhd->brd", gate_blocks, gate_table) + jnp.einsum("rbh,bhd->brd", up_blocks, up_table)
        partial_value = lax.optimization_barrier(partial_value.astype(jnp.bfloat16)).astype(jnp.float32)
        route_grad = jnp.sum(partial_value, axis=0).astype(jnp.bfloat16)
        return gate_wgrad, up_wgrad, down_wgrad, route_grad

    w_gate_grad, w_up_grad, w_down_grad, route_grads = lax.map(expert, (order, w_gate, w_up, w_down))
    placed = jnp.zeros((TOKENS * TOPK, D), jnp.float32).at[order.reshape(-1)].set(route_grads.reshape(-1, D).astype(jnp.float32))
    moe_in_grad = jnp.sum(placed.reshape(TOKENS, TOPK, D), axis=1).astype(jnp.bfloat16)

    stream_grad = (cotangent.astype(jnp.float32) + moe_in_grad.astype(jnp.float32)).astype(jnp.bfloat16)
    mixed_in = lax.optimization_barrier((gate_c.astype(jnp.float32) * value_x.astype(jnp.float32)).astype(jnp.bfloat16))
    extended = jnp.pad(mixed_in.astype(jnp.float32), ((0, 0), (TAPS - 1, 0)))
    conv_out = jnp.zeros((W_A, TOKENS), jnp.float32)
    for tap in range(TAPS):
        conv_out = conv_out + conv_taps[tap][:, None] * extended[:, tap:tap + TOKENS]
    mixer_act = (gate_b.astype(jnp.float32) * conv_out).astype(jnp.bfloat16)
    act_grad = lax.dot_general(out_proj, stream_grad, contract_model, preferred_element_type=jnp.float32)
    proj_grad = jnp.dot(mixer_act, stream_grad, preferred_element_type=jnp.float32)
    gate_b_grad = (act_grad * conv_out).astype(jnp.bfloat16)
    conv_grad = act_grad * gate_b.astype(jnp.float32)
    extended_grad = jnp.pad(conv_grad, ((0, 0), (0, TAPS - 1)))
    mixed_grad = jnp.zeros((W_A, TOKENS), jnp.float32)
    for tap in range(TAPS):
        offset = TAPS - 1 - tap
        mixed_grad = mixed_grad + conv_taps[tap][:, None] * extended_grad[:, offset:offset + TOKENS]
    gate_c_grad = (mixed_grad * value_x.astype(jnp.float32)).astype(jnp.bfloat16)
    value_x_grad = (mixed_grad * gate_c.astype(jnp.float32)).astype(jnp.bfloat16)
    return (w_gate_grad, w_up_grad, w_down_grad, moe_in_grad, proj_grad, gate_b_grad, gate_c_grad, value_x_grad)
```

```python
import jax
import jax.numpy as jnp
from jax import lax
from jax.sharding import Mesh
from jax.sharding import PartitionSpec as P

TAPS = 3
GROUPS = 4
CORES = 2
BF = jnp.bfloat16
F32 = jnp.float32
SP = ("z", "c")


def from_behind(array, by):
    count = lax.axis_size(SP)
    pairs = [(i, i + by) for i in range(count) if 0 <= i + by < count]
    return lax.ppermute(array, SP, pairs)


def partner(array, axis, bit):
    count = lax.axis_size(axis)
    return lax.ppermute(array, axis, [(i, i ^ bit) for i in range(count)])


def dot(a, b, ca, cb, kind=F32):
    return lax.dot_general(a, b, (((ca,), (cb,)), ((), ())), preferred_element_type=F32).astype(kind)


def shared_plan(sp, tp, top_routes):
    return top_routes == CORES and GROUPS * CORES == sp and tp == GROUPS and tp & (tp - 1) == 0


def shared_rows(
    moe_in, cotangent, routing, route_weight, w_gate, w_up, w_down,
    gate_b, gate_c, value_x, conv_taps, out_proj,
):
    planes = lax.axis_size("z")
    lanes = lax.axis_size("tp")
    z, c, l = lax.axis_index("z"), lax.axis_index("c"), lax.axis_index("tp")
    rows, width = moe_in.shape
    cap = rows // planes
    cols = width // lanes
    half = cols // CORES
    at = l * cols

    group = routing[:, 0] // CORES
    hot = (group[:, None] == jnp.arange(planes)[None, :]).astype(BF)
    t = jnp.arange(rows)
    before = (t[:, None] > t[None, :]).astype(BF)
    rank = jnp.sum(dot(before, hot, 1, 0) * hot.astype(F32), axis=1).astype(jnp.int32)
    place = group * cap + rank
    perm = (place[:, None] == t[None, :]).astype(BF)

    core = routing % CORES
    weights = [jnp.sum(jnp.where(core == k, route_weight, 0.0), axis=1) for k in range(CORES)]
    weights = jnp.stack(weights, axis=1)
    high = weights.astype(BF)
    low = (weights - high.astype(F32)).astype(BF)
    parts = dot(jnp.concatenate([high, low], axis=1), perm, 0, 0, BF)
    parts = parts.reshape(2 * CORES, planes, cap).transpose(1, 0, 2).reshape(planes, 1, 2 * CORES * cap)
    parts = jnp.pad(parts, ((0, 0), (0, 15), (0, cols - 2 * CORES * cap)))

    x_rows = dot(perm, lax.dynamic_slice_in_dim(moe_in, at, cols, 1), 0, 0, BF)
    c_rows = dot(perm, lax.dynamic_slice_in_dim(cotangent, at, cols, 1), 0, 0, BF)
    sent = jnp.concatenate(
        [x_rows.reshape(planes, cap, cols), c_rows.reshape(planes, cap, cols), parts], axis=1
    )

    def over_planes(blocks):
        own = lax.dynamic_index_in_dim(blocks, z, 0, False)
        return [own] + [
            partner(lax.dynamic_index_in_dim(blocks, z ^ bit, 0, False), "z", bit)
            for bit in range(1, planes)
        ]

    got = over_planes(sent)
    x_own = jnp.concatenate([g[:cap] for g in got], axis=0)
    c_own = jnp.concatenate([g[cap : 2 * cap] for g in got], axis=0)
    w_own = jnp.concatenate(
        [g[2 * cap, : 2 * CORES * cap].reshape(2, CORES, cap) for g in got], axis=2
    ).astype(F32)
    w_own = w_own[0] + w_own[1]
    w_mine = lax.dynamic_index_in_dim(w_own, c, 0, False)
    w_other = lax.dynamic_index_in_dim(w_own, 1 - c, 0, False)
    w_far = partner(w_other, "c", 1)
    scale = jnp.concatenate([w_mine, w_far])[:, None]

    def over_lanes(piece):
        a, b = partner(piece, "tp", 1), partner(piece, "tp", 2)
        m = piece.shape[0] // 2
        d = jnp.concatenate([partner(b[:m], "tp", 1), partner(a[m:], "tp", 2)], axis=0)
        return [piece, a, b, d]

    def join(pieces):
        out = jnp.zeros((pieces[0].shape[0], width), pieces[0].dtype)
        for bit, piece in enumerate(pieces):
            out = lax.dynamic_update_slice_in_dim(out, piece, (l ^ bit) * cols, 1)
        return out

    x_near = join(over_lanes(x_own))
    c_near = join(over_lanes(c_own))
    arrived = jnp.concatenate([x_near, partner(x_near, "c", 1)], axis=0)
    arrived_cot = jnp.concatenate([c_near, partner(c_near, "c", 1)], axis=0)

    gate_pre = dot(arrived, w_gate[0], 1, 1)
    up_pre = dot(arrived, w_up[0], 1, 1)
    sig = jax.nn.sigmoid(gate_pre)
    hidden = gate_pre * sig * up_pre
    hidden_grad = scale * dot(arrived_cot, w_down[0], 1, 1)
    gate_grad = (hidden_grad * up_pre * sig * (1.0 + gate_pre * (1.0 - sig))).astype(BF)
    up_grad = (hidden_grad * gate_pre * sig).astype(BF)
    scaled_hidden = (scale * hidden).astype(BF)
    partial = dot(gate_grad, w_gate[0], 1, 0) + dot(up_grad, w_up[0], 1, 0)
    w_gate_grad = dot(gate_grad, arrived, 0, 0, BF)[None]
    w_up_grad = dot(up_grad, arrived, 0, 0, BF)[None]
    w_down_grad = dot(scaled_hidden, arrived_cot, 0, 0, BF)[None]

    partial = partial.astype(BF)
    near = partial[:rows].astype(F32) + partner(partial[rows:], "c", 1).astype(F32)
    near = near.astype(BF)
    total = lax.dynamic_slice_in_dim(near, at, cols, 1).astype(F32)
    for bit in range(1, lanes):
        piece = lax.dynamic_slice_in_dim(near, (l ^ bit) * cols, cols, 1)
        total = total + partner(piece, "tp", bit).astype(F32)
    total = total.astype(BF).reshape(planes, cap, cols)
    back = [total[0]] + [partner(total[bit], "z", bit) for bit in range(1, planes)]
    placed = jnp.stack(back)
    order = z ^ jnp.arange(planes)
    sorted_grad = jnp.zeros((planes, cap, cols), BF)
    for bit in range(planes):
        sorted_grad = lax.dynamic_update_index_in_dim(sorted_grad, back[bit], z ^ bit, 0)
    moe_in_grad = dot(perm, sorted_grad.reshape(rows, cols), 1, 0, BF)

    mixed_in = (gate_c.astype(F32) * value_x.astype(F32)).astype(BF)
    earlier = from_behind(mixed_in[:, rows - (TAPS - 1) :], 1)
    extended = jnp.concatenate([earlier, mixed_in], axis=1).astype(F32)
    conv_out = jnp.zeros(mixed_in.shape, F32)
    for tap in range(TAPS):
        conv_out = conv_out + conv_taps[tap][:, None] * extended[:, tap : tap + rows]
    mixer_act = (gate_b.astype(F32) * conv_out).astype(BF)
    acts = jnp.stack([mixer_act] + [partner(mixer_act, "tp", bit) for bit in range(1, lanes)])

    cot_part = lax.dynamic_slice_in_dim(cotangent, at, cols, 1)
    stream_part = (cot_part.astype(F32) + moe_in_grad.astype(F32)).astype(BF)
    share = dot(acts.reshape(-1, rows), stream_part, 1, 0).reshape(lanes, -1, cols)
    share_far = lax.dynamic_slice_in_dim(share, (1 - c) * half, half, 2).astype(BF)
    share_near = lax.dynamic_slice_in_dim(share, c * half, half, 2)
    share = (share_near + partner(share_far, "c", 1).astype(F32)).astype(BF)
    proj_grad = jnp.zeros(share.shape[1:], F32)
    for turn in range(lanes):
        piece = lax.dynamic_index_in_dim(share, l ^ z ^ turn, 0, False)
        pairs = [
            (a * lanes + b, b * lanes + (a ^ turn)) for a in range(planes) for b in range(lanes)
        ]
        proj_grad = proj_grad + lax.ppermute(piece, ("z", "tp"), pairs).astype(F32)

    full_grad = join([moe_in_grad] + [partner(moe_in_grad, "tp", bit) for bit in range(1, lanes)])
    stream_grad = (cotangent.astype(F32) + full_grad.astype(F32)).astype(BF)
    act_grad = dot(out_proj, stream_grad, 1, 1)
    gate_b_grad = (act_grad * conv_out).astype(BF)
    conv_grad = act_grad * gate_b.astype(F32)
    later = from_behind(conv_grad[:, : TAPS - 1], -1)
    extended_grad = jnp.concatenate([conv_grad, later], axis=1)
    mixed_grad = jnp.zeros(conv_grad.shape, F32)
    for tap in range(TAPS):
        offset = TAPS - 1 - tap
        mixed_grad = mixed_grad + conv_taps[tap][:, None] * extended_grad[:, offset : offset + rows]
    gate_c_grad = (mixed_grad * value_x.astype(F32)).astype(BF)
    value_x_grad = (mixed_grad * gate_c.astype(F32)).astype(BF)
    return (
        w_gate_grad, w_up_grad, w_down_grad, moe_in_grad, proj_grad,
        gate_b_grad, gate_c_grad, value_x_grad,
    )


def any_rows(
    moe_in, cotangent, routing, route_weight, w_gate, w_up, w_down,
    gate_b, gate_c, value_x, conv_taps, out_proj,
):
    tok_rows, top_routes = routing.shape
    experts = lax.axis_size(SP)
    lane_count = lax.axis_size("tp")
    model_width = moe_in.shape[1]
    capacity = top_routes * tok_rows // experts
    flat_routes = routing.reshape(-1)
    route_count = flat_routes.shape[0]
    one_hot = (flat_routes[:, None] == jnp.arange(experts, dtype=jnp.int32)[None, :]).astype(
        jnp.int32
    )
    slot_rank = jnp.sum(jnp.cumsum(one_hot, axis=0) * one_hot, axis=1) - 1
    slot_index = flat_routes * capacity + slot_rank
    source = (
        jnp.zeros((route_count,), jnp.int32)
        .at[slot_index]
        .set(jnp.arange(route_count, dtype=jnp.int32))
    )
    owner_token = source // top_routes
    scales = route_weight.reshape(-1)[source][:, None]
    col_width = model_width // lane_count
    col_start = lax.axis_index("tp") * col_width
    rows_part = lax.dynamic_slice_in_dim(moe_in, col_start, col_width, 1)[owner_token]
    cot_slice = lax.dynamic_slice_in_dim(cotangent, col_start, col_width, 1)[owner_token]
    cot_part = (scales * cot_slice.astype(F32)).astype(BF)
    moved = (
        lax.all_to_all(rows_part, SP, split_axis=0, concat_axis=0, tiled=True),
        lax.all_to_all(cot_part, SP, split_axis=0, concat_axis=0, tiled=True),
    )
    arrived, arrived_cot = (
        lax.all_gather(moved[0], "tp", axis=1, tiled=True),
        lax.all_gather(moved[1], "tp", axis=1, tiled=True),
    )
    gate_pre = dot(arrived, w_gate[0], 1, 1)
    up_pre = dot(arrived, w_up[0], 1, 1)
    sigmoid_gate = jax.nn.sigmoid(gate_pre)
    hidden = (gate_pre * sigmoid_gate * up_pre).astype(BF)
    hidden_grad = dot(arrived_cot, w_down[0], 1, 1)
    gate_grad = (
        hidden_grad * up_pre * sigmoid_gate * (1.0 + gate_pre * (1.0 - sigmoid_gate))
    ).astype(BF)
    up_grad = (hidden_grad * gate_pre * sigmoid_gate).astype(BF)
    w_gate_grad = dot(gate_grad, arrived, 0, 0, BF)[None]
    w_up_grad = dot(up_grad, arrived, 0, 0, BF)[None]
    w_down_grad = dot(hidden, arrived_cot, 0, 0, BF)[None]
    partial_value = dot(gate_grad, w_gate[0], 1, 0) + dot(up_grad, w_up[0], 1, 0)
    summed = lax.psum_scatter(partial_value.astype(BF), "tp", scatter_dimension=1, tiled=True)
    returned = lax.all_to_all(summed, SP, split_axis=0, concat_axis=0, tiled=True)
    per_route = returned[slot_index].astype(F32)
    moe_in_grad = jnp.sum(per_route.reshape(tok_rows, top_routes, -1), axis=1).astype(BF)
    full_grad = lax.all_gather(moe_in_grad, "tp", axis=1, tiled=True)
    stream_grad = (cotangent.astype(F32) + full_grad.astype(F32)).astype(BF)
    mixed_in = (gate_c.astype(F32) * value_x.astype(F32)).astype(BF)
    earlier = from_behind(mixed_in[:, tok_rows - (TAPS - 1) :], 1)
    extended = jnp.concatenate([earlier, mixed_in], axis=1).astype(F32)
    conv_out = jnp.zeros(mixed_in.shape, F32)
    for tap in range(TAPS):
        conv_out = conv_out + conv_taps[tap][:, None] * extended[:, tap : tap + tok_rows]
    mixer_act = (gate_b.astype(F32) * conv_out).astype(BF)
    act_grad = dot(out_proj, stream_grad, 1, 1)
    proj_rows = lax.psum_scatter(
        dot(stream_grad, mixer_act, 0, 1, BF), SP, scatter_dimension=0, tiled=True
    ).astype(F32)
    proj_grad = proj_rows.T
    gate_b_grad = (act_grad * conv_out).astype(BF)
    conv_grad = act_grad * gate_b.astype(F32)
    later = from_behind(conv_grad[:, : TAPS - 1], -1)
    extended_grad = jnp.concatenate([conv_grad, later], axis=1)
    mixed_grad = jnp.zeros(conv_grad.shape, F32)
    for tap in range(TAPS):
        offset = TAPS - 1 - tap
        mixed_grad = (
            mixed_grad + conv_taps[tap][:, None] * extended_grad[:, offset : offset + tok_rows]
        )
    gate_c_grad = (mixed_grad * value_x.astype(F32)).astype(BF)
    value_x_grad = (mixed_grad * gate_c.astype(F32)).astype(BF)
    return (
        w_gate_grad, w_up_grad, w_down_grad, moe_in_grad, proj_grad,
        gate_b_grad, gate_c_grad, value_x_grad,
    )


def solution(mesh):
    sp, tp = mesh.shape["sp"], mesh.shape["tp"]
    split = Mesh(mesh.devices.reshape(sp // CORES, CORES, tp), ("z", "c", "tp"))
    experts = P(SP, "tp", None)
    tokens = P(SP, None)
    mixer = P("tp", SP)

    def step(moe_in, cotangent, routing, *rest):
        body = shared_rows if shared_plan(sp, tp, routing.shape[1]) else any_rows
        return jax.shard_map(
            body,
            mesh=split,
            in_specs=(tokens,) * 4 + (experts,) * 3 + (mixer,) * 3 + (P(None, "tp"), P("tp", None)),
            out_specs=(experts,) * 3 + (P(SP, "tp"),) + (mixer,) * 4,
            check_vma=False,
        )(moe_in, cotangent, routing, *rest)

    return step
```

```python
import functools

import jax
import jax.numpy as jnp
from jax import lax
from jax.experimental import pallas as pl
from jax.experimental.pallas import tpu as pltpu
from jax.sharding import Mesh
from jax.sharding import PartitionSpec as P

TAPS = 3
GROUPS = 4
CORES = 2
BF = jnp.bfloat16
F32 = jnp.float32
SP = ("z", "c")
EXTRA = 16


def from_behind(array, by):
    count = lax.axis_size(SP)
    pairs = [(i, i + by) for i in range(count) if 0 <= i + by < count]
    return lax.ppermute(array, SP, pairs)


def partner(array, axis, bit):
    count = lax.axis_size(axis)
    return lax.ppermute(array, axis, [(i, i ^ bit) for i in range(count)])


def dot(a, b, ca, cb, kind=F32):
    return lax.dot_general(a, b, (((ca,), (cb,)), ((), ())), preferred_element_type=F32).astype(kind)


def shared_plan(sp, tp, top_routes):
    return top_routes == CORES and GROUPS * CORES == sp and tp == GROUPS and tp & (tp - 1) == 0


def iota(shape, axis):
    return lax.broadcasted_iota(jnp.int32, shape, axis)


def call(kernel, outs, flops, moved, *args):
    return pl.pallas_call(
        kernel,
        out_shape=outs,
        cost_estimate=pl.CostEstimate(flops=flops, bytes_accessed=moved, transcendentals=0),
        compiler_params=pltpu.CompilerParams(vmem_limit_bytes=48 * 1024 * 1024),
    )(*args)


def shape(*dims, kind=BF):
    return jax.ShapeDtypeStruct(dims, kind)


def sort_kernel(planes, cap, cols, routing_ref, weight_ref, x_ref, c_ref, sent_ref, perm_ref):
    rows = planes * cap
    z, l = lax.axis_index("z"), lax.axis_index("tp")
    routing = routing_ref[...]
    lane = iota((rows, 128), 1)
    first = CORES * jnp.bitwise_xor(lane, z)
    group = routing[:, :1]
    hot = (group >= first) & (group < first + CORES) & (lane < planes)
    before = (iota((rows, rows), 0) > iota((rows, rows), 1)).astype(F32).astype(BF)
    rank = dot(before, hot.astype(F32).astype(BF), 1, 0)
    place = jnp.sum(
        jnp.where(hot, rank + (lane * cap).astype(F32), 0.0), axis=1, keepdims=True
    )
    perm = (place.astype(jnp.int32) == iota((rows, rows), 1)).astype(F32).astype(BF)
    perm_ref[...] = perm
    part = pl.ds(pl.multiple_of(l * cols, cols), cols)
    x = dot(perm, x_ref[:, part], 0, 0, BF)
    cot = dot(perm, c_ref[:, part], 0, 0, BF)
    core = jnp.bitwise_and(routing, CORES - 1)
    weight = weight_ref[...]
    table = jnp.zeros((rows, 128), F32)
    for k in range(CORES):
        w = jnp.sum(jnp.where(core == k, weight, 0.0), axis=1, keepdims=True)
        high = w.astype(BF).astype(F32)
        table = jnp.where(lane == k, high, jnp.where(lane == CORES + k, w - high, table))
    parts = dot(table.astype(BF), perm, 0, 0)[:EXTRA].astype(BF)
    for b in range(planes):
        sent_ref[b, :cap, :] = x[b * cap : (b + 1) * cap]
        sent_ref[b, cap : 2 * cap, :] = cot[b * cap : (b + 1) * cap]
        sent_ref[b, 2 * cap :, :] = jnp.zeros((EXTRA, cols), BF)
        sent_ref[b, 2 * cap :, :rows] = parts


def expert_kernel(planes, cap, cols, *refs):
    pieces, (extras, wg_ref, wu_ref, wd_ref) = (refs[:5], refs[5:10]), (refs[10:12], *refs[12:15])
    x_ref, c_ref, gg_ref, ug_ref, sh_ref, near_ref, far_ref = refs[15:22]
    rows = planes * cap
    c, l = lax.axis_index("c"), lax.axis_index("tp")
    lane = iota((cap, rows), 1)
    row = iota((cap, rows), 0)
    scales = []
    for side in range(2):
        own, one, two, low, high = pieces[side]
        for k, piece in enumerate((own, one, two, None)):
            to = pl.ds(pl.multiple_of(jnp.bitwise_xor(l, k) * cols, cols), cols)
            for b in range(planes):
                part = piece[b] if piece is not None else (low[b] if b < planes // 2 else high[b - planes // 2])
                at = pl.ds(side * rows + b * cap, cap)
                x_ref[at, to] = part[:cap]
                c_ref[at, to] = part[cap:]
        for b in range(planes):
            extra = extras[side][b].astype(F32)
            w = extra[:CORES, :rows] + extra[CORES : 2 * CORES, :rows]
            w = jnp.where(c == 0, w[:1], w[1:2])
            scales.append(jnp.sum(jnp.where(lane == row + b * cap, w, 0.0), axis=1, keepdims=True))
    scale = jnp.concatenate(scales, axis=0)
    hid = wg_ref.shape[0]
    step = 256

    @pl.loop(0, hid // step)
    def _(i):
        at = pl.ds(pl.multiple_of(i * step, step), step)
        gate = dot(x_ref[...], wg_ref[at, :], 1, 1)
        up = dot(x_ref[...], wu_ref[at, :], 1, 1)
        back = scale * dot(c_ref[...], wd_ref[at, :], 1, 1)
        sig = jax.nn.sigmoid(gate)
        act = gate * sig
        gg_ref[:, at] = (back * up * sig * (1.0 + gate * (1.0 - sig))).astype(BF)
        ug_ref[:, at] = (back * act).astype(BF)
        sh_ref[:, at] = (scale * act * up).astype(BF)

    lanes = wg_ref.shape[1] // cols

    @pl.loop(0, lanes)
    def _(k):
        at = pl.ds(pl.multiple_of(jnp.bitwise_xor(l, k) * cols, cols), cols)
        out = dot(gg_ref[...], wg_ref[:, at], 1, 0) + dot(ug_ref[...], wu_ref[:, at], 1, 0)
        near_ref[k] = out[:rows].astype(BF)
        far_ref[k] = out[rows:].astype(BF)


def tail_kernel(planes, cols, own, one, two, three, cot_ref, mixer_ref, out_ref, near_ref, far_ref, act_ref, stream):
    z, c, l = lax.axis_index("z"), lax.axis_index("c"), lax.axis_index("tp")
    for k, piece in enumerate((own, one, two, three)):
        at = pl.ds(pl.multiple_of(jnp.bitwise_xor(l, k) * cols, cols), cols)
        stream[:, at] = (cot_ref[:, at].astype(F32) + piece[...].astype(F32)).astype(BF)
    half = cols // CORES
    for b in range(planes):
        for ref, core in ((near_ref, c), (far_ref, 1 - c)):
            at = (jnp.bitwise_xor(z, b) * CORES + core) * half
            ref[b] = dot(mixer_ref[...], stream[:, pl.ds(pl.multiple_of(at, half), half)], 1, 0).astype(ref.dtype)
    act_ref[...] = dot(out_ref[...], stream[...], 1, 1)


def shared_rows(
    moe_in, cotangent, routing, route_weight, w_gate, w_up, w_down,
    gate_b, gate_c, value_x, conv_taps, out_proj,
):
    planes = lax.axis_size("z")
    lanes = lax.axis_size("tp")
    rows, width = moe_in.shape
    cap = rows // planes
    cols = width // lanes
    hid = w_gate.shape[1]
    chans = out_proj.shape[0]

    sent, perm = call(
        functools.partial(sort_kernel, planes, cap, cols),
        (shape(planes, 2 * cap + EXTRA, cols), shape(rows, rows)),
        4 * rows * rows * cols, 4 * rows * width * 2,
        routing, route_weight, moe_in, cotangent,
    )
    got = [sent[0]] + [partner(sent[b], "z", b) for b in range(1, planes)]
    own = jnp.stack([g[: 2 * cap] for g in got])
    extra = jnp.stack([g[2 * cap :] for g in got])
    one, two = partner(own, "tp", 1), partner(own, "tp", 2)
    half = planes // 2
    low, high = partner(two[:half], "tp", 1), partner(one[half:], "tp", 2)
    near = [own, one, two, low, high]
    far = [partner(piece, "c", 1) for piece in near]
    both = 2 * rows
    x, cot, gate_grad, up_grad, hidden, p_near, p_far = call(
        functools.partial(expert_kernel, planes, cap, cols),
        (shape(both, width), shape(both, width)) + (shape(both, hid),) * 3
        + (shape(lanes, rows, cols),) * 2,
        10 * both * hid * width, 12 * hid * width,
        *near, *far, extra, partner(extra, "c", 1), w_gate[0], w_up[0], w_down[0],
    )
    w_gate_grad = dot(gate_grad, x, 0, 0, BF)[None]
    w_up_grad = dot(up_grad, x, 0, 0, BF)[None]
    w_down_grad = dot(hidden, cot, 0, 0, BF)[None]

    p_sum = (p_near.astype(F32) + partner(p_far, "c", 1).astype(F32)).astype(BF)
    total = p_sum[0].astype(F32)
    for b in range(1, lanes):
        total = total + partner(p_sum[b], "tp", b).astype(F32)
    total = total.astype(BF).reshape(planes, cap, cols)
    back = [total[0]] + [partner(total[b], "z", b) for b in range(1, planes)]
    moe_in_grad = dot(perm, jnp.concatenate(back, axis=0), 1, 0, BF)

    mixed_in = (gate_c.astype(F32) * value_x.astype(F32)).astype(BF)
    earlier = from_behind(mixed_in[:, rows - (TAPS - 1) :], 1)
    extended = jnp.concatenate([earlier, mixed_in], axis=1).astype(F32)
    conv_out = jnp.zeros(mixed_in.shape, F32)
    for tap in range(TAPS):
        conv_out = conv_out + conv_taps[tap][:, None] * extended[:, tap : tap + rows]
    mixer_act = (gate_b.astype(F32) * conv_out).astype(BF)

    part = cols // CORES
    q_near, q_far, act_grad = pl.pallas_call(
        functools.partial(tail_kernel, planes, cols),
        out_shape=(
            shape(planes, chans, part, kind=F32), shape(planes, chans, part), shape(chans, rows, kind=F32),
        ),
        scratch_shapes=[pltpu.VMEM((rows, width), BF)],
        cost_estimate=pl.CostEstimate(flops=4 * chans * rows * width, bytes_accessed=6 * rows * width, transcendentals=0),
        compiler_params=pltpu.CompilerParams(vmem_limit_bytes=24 * 1024 * 1024),
    )(
        moe_in_grad, *[partner(moe_in_grad, "tp", b) for b in range(1, lanes)],
        cotangent, mixer_act, out_proj,
    )
    q_sum = q_near + partner(q_far, "c", 1).astype(F32)
    proj_grad = q_sum[0]
    for b in range(1, planes):
        proj_grad = proj_grad + partner(q_sum[b].astype(BF), "z", b).astype(F32)

    gate_b_grad = (act_grad * conv_out).astype(BF)
    conv_grad = act_grad * gate_b.astype(F32)
    later = from_behind(conv_grad[:, : TAPS - 1], -1)
    extended_grad = jnp.concatenate([conv_grad, later], axis=1)
    mixed_grad = jnp.zeros(conv_grad.shape, F32)
    for tap in range(TAPS):
        offset = TAPS - 1 - tap
        mixed_grad = mixed_grad + conv_taps[tap][:, None] * extended_grad[:, offset : offset + rows]
    gate_c_grad = (mixed_grad * value_x.astype(F32)).astype(BF)
    value_x_grad = (mixed_grad * gate_c.astype(F32)).astype(BF)
    return (
        w_gate_grad, w_up_grad, w_down_grad, moe_in_grad, proj_grad,
        gate_b_grad, gate_c_grad, value_x_grad,
    )


def any_rows(
    moe_in, cotangent, routing, route_weight, w_gate, w_up, w_down,
    gate_b, gate_c, value_x, conv_taps, out_proj,
):
    tok_rows, top_routes = routing.shape
    experts = lax.axis_size(SP)
    lane_count = lax.axis_size("tp")
    model_width = moe_in.shape[1]
    capacity = top_routes * tok_rows // experts
    flat_routes = routing.reshape(-1)
    route_count = flat_routes.shape[0]
    one_hot = (flat_routes[:, None] == jnp.arange(experts, dtype=jnp.int32)[None, :]).astype(
        jnp.int32
    )
    slot_rank = jnp.sum(jnp.cumsum(one_hot, axis=0) * one_hot, axis=1) - 1
    slot_index = flat_routes * capacity + slot_rank
    source = (
        jnp.zeros((route_count,), jnp.int32)
        .at[slot_index]
        .set(jnp.arange(route_count, dtype=jnp.int32))
    )
    owner_token = source // top_routes
    scales = route_weight.reshape(-1)[source][:, None]
    col_width = model_width // lane_count
    col_start = lax.axis_index("tp") * col_width
    rows_part = lax.dynamic_slice_in_dim(moe_in, col_start, col_width, 1)[owner_token]
    cot_slice = lax.dynamic_slice_in_dim(cotangent, col_start, col_width, 1)[owner_token]
    cot_part = (scales * cot_slice.astype(F32)).astype(BF)
    moved = (
        lax.all_to_all(rows_part, SP, split_axis=0, concat_axis=0, tiled=True),
        lax.all_to_all(cot_part, SP, split_axis=0, concat_axis=0, tiled=True),
    )
    arrived, arrived_cot = (
        lax.all_gather(moved[0], "tp", axis=1, tiled=True),
        lax.all_gather(moved[1], "tp", axis=1, tiled=True),
    )
    gate_pre = dot(arrived, w_gate[0], 1, 1)
    up_pre = dot(arrived, w_up[0], 1, 1)
    sigmoid_gate = jax.nn.sigmoid(gate_pre)
    hidden = (gate_pre * sigmoid_gate * up_pre).astype(BF)
    hidden_grad = dot(arrived_cot, w_down[0], 1, 1)
    gate_grad = (
        hidden_grad * up_pre * sigmoid_gate * (1.0 + gate_pre * (1.0 - sigmoid_gate))
    ).astype(BF)
    up_grad = (hidden_grad * gate_pre * sigmoid_gate).astype(BF)
    w_gate_grad = dot(gate_grad, arrived, 0, 0, BF)[None]
    w_up_grad = dot(up_grad, arrived, 0, 0, BF)[None]
    w_down_grad = dot(hidden, arrived_cot, 0, 0, BF)[None]
    partial_value = dot(gate_grad, w_gate[0], 1, 0) + dot(up_grad, w_up[0], 1, 0)
    summed = lax.psum_scatter(partial_value.astype(BF), "tp", scatter_dimension=1, tiled=True)
    returned = lax.all_to_all(summed, SP, split_axis=0, concat_axis=0, tiled=True)
    per_route = returned[slot_index].astype(F32)
    moe_in_grad = jnp.sum(per_route.reshape(tok_rows, top_routes, -1), axis=1).astype(BF)
    full_grad = lax.all_gather(moe_in_grad, "tp", axis=1, tiled=True)
    stream_grad = (cotangent.astype(F32) + full_grad.astype(F32)).astype(BF)
    mixed_in = (gate_c.astype(F32) * value_x.astype(F32)).astype(BF)
    earlier = from_behind(mixed_in[:, tok_rows - (TAPS - 1) :], 1)
    extended = jnp.concatenate([earlier, mixed_in], axis=1).astype(F32)
    conv_out = jnp.zeros(mixed_in.shape, F32)
    for tap in range(TAPS):
        conv_out = conv_out + conv_taps[tap][:, None] * extended[:, tap : tap + tok_rows]
    mixer_act = (gate_b.astype(F32) * conv_out).astype(BF)
    act_grad = dot(out_proj, stream_grad, 1, 1)
    proj_rows = lax.psum_scatter(
        dot(stream_grad, mixer_act, 0, 1, BF), SP, scatter_dimension=0, tiled=True
    ).astype(F32)
    proj_grad = proj_rows.T
    gate_b_grad = (act_grad * conv_out).astype(BF)
    conv_grad = act_grad * gate_b.astype(F32)
    later = from_behind(conv_grad[:, : TAPS - 1], -1)
    extended_grad = jnp.concatenate([conv_grad, later], axis=1)
    mixed_grad = jnp.zeros(conv_grad.shape, F32)
    for tap in range(TAPS):
        offset = TAPS - 1 - tap
        mixed_grad = (
            mixed_grad + conv_taps[tap][:, None] * extended_grad[:, offset : offset + tok_rows]
        )
    gate_c_grad = (mixed_grad * value_x.astype(F32)).astype(BF)
    value_x_grad = (mixed_grad * gate_c.astype(F32)).astype(BF)
    return (
        w_gate_grad, w_up_grad, w_down_grad, moe_in_grad, proj_grad,
        gate_b_grad, gate_c_grad, value_x_grad,
    )


def solution(mesh):
    sp, tp = mesh.shape["sp"], mesh.shape["tp"]
    split = Mesh(mesh.devices.reshape(sp // CORES, CORES, tp), ("z", "c", "tp"))
    experts = P(SP, "tp", None)
    tokens = P(SP, None)
    mixer = P("tp", SP)

    def step(moe_in, cotangent, routing, *rest):
        body = shared_rows if shared_plan(sp, tp, routing.shape[1]) else any_rows
        return jax.shard_map(
            body,
            mesh=split,
            in_specs=(tokens,) * 4 + (experts,) * 3 + (mixer,) * 3 + (P(None, "tp"), P("tp", None)),
            out_specs=(experts,) * 3 + (P(SP, "tp"),) + (mixer,) * 4,
            check_vma=False,
        )(moe_in, cotangent, routing, *rest)

    return step
```
